32 devices in a mesh: kv: 8 (over z, y), tp: 4 (over x, core).
Axes of the slice: x: 2, y: 2, z: 4, core: 2. Of those that a mesh axis runs over, the one named last changes fastest.
Arguments:
- proposals: bfloat16 [16, 4, 4096], P('kv', None, 'tp'), may hold values from -6 to 6
- input_norm_gain: float32 [4096], replicated, may hold values from 0.1 to 1.9
- query_matrix: bfloat16 [4096, 2048], P(None, 'tp'), may hold values from -0.09375 to 0.09375
- forget_gate_matrix: bfloat16 [4096, 2048], P(None, 'tp'), may hold values from -0.09375 to 0.09375
- value_matrix: bfloat16 [4096, 2048], P(None, 'tp'), may hold values from -0.09375 to 0.09375
- forget_floor_channel: float32 [2048], P('tp'), may hold values from 0.02 to 0.95
- proposal_extra_decay: float32 [16, 4, 16], P('kv', None, 'tp'), may hold values from -0.7 to 0
- prior_proposal_states: float32 [16, 4, 2048, 128], P('kv', None, 'tp'), may hold values from -4 to 4
- accepted: int32 [16], P('kv'), may hold values from 1 to 4
- output_matrix: bfloat16 [2048, 4096], P('tp', 'kv'), may hold values from -0.02734375 to 0.02734375
Outputs:
- mixer_output: bfloat16 [16, 4, 4096], P('tp', None, 'kv')
- next_states: float32 [16, 4, 2048, 128], P('kv', None, 'tp')
The draws below stay inside these ranges and needn't reach their ends.
All inputs are finite; a program needn't handle non-finite values.
Results may differ from the reference program's by a relative error of at most 0.012.
Values may be sent and summed in bfloat16 or wider, within the bound.
A program may use at most 64 MiB of HBM per device.

```python
import jax
import jax.numpy as jnp
from jax import lax

D = 4096
HEADS = 16
HEAD_DIM = 128
PROPOSALS = 4
SEQS = 16


def draw_proposal_extra_decay(key, part):
    first_key, second_key = jax.random.split(jax.random.fold_in(key, 7))
    hitting = jax.random.uniform(first_key, (SEQS, PROPOSALS, HEADS), jnp.float32) < 0.2
    keeping = jax.random.uniform(second_key, (SEQS, PROPOSALS, HEADS), jnp.float32, minval=0.5, maxval=0.8)
    return jnp.where(hitting, jnp.log(keeping), 0.0).astype(jnp.float32)


def plant(array, stream_key, smallest, top_value):
    shape = array.shape
    index_at = [jax.random.randint(jax.random.fold_in(stream_key, axis), (), 0, shape[axis]) for axis in range(len(shape))]
    array = array.at[tuple(index_at)].set(smallest)
    longest = shape.index(max(shape))
    index_at[longest] = (index_at[longest] + 1) % shape[longest]
    return array.at[tuple(index_at)].set(top_value)


def levels(rng, shape, pieces, low, largest):
    level = 1.0
    for axis_at, shards_of in pieces:
        draws = jax.random.uniform(jax.random.fold_in(jax.random.fold_in(rng, 6), axis_at), (shards_of,), jnp.float32, low / len(pieces), largest / len(pieces))
        level = level * jnp.repeat(jnp.exp(draws), shape[axis_at] // shards_of).reshape((-1,) + (1,) * (len(shape) - 1 - axis_at))
    return level


def scatter_about(key, shape, deviation, limit, cuts=(), held_as=jnp.bfloat16):
    values = jax.random.normal(key, shape, jnp.float32) * deviation
    if len(cuts) > 0:
        values = levels(key, shape, cuts, -0.22, 0.18) * values
    return jnp.clip(values, min=-limit, max=limit).astype(held_as)


def setup_inputs(seed: int = 0) -> dict:
    key_list = jax.random.split(jax.random.key(seed), 11)
    proposals = scatter_about(key_list[0], (SEQS, PROPOSALS, D), 1.0, 6.0, ((0, 8), (2, 4)))
    input_norm_gain = jnp.clip(1.0 + 0.18 * jax.random.normal(key_list[1], (D,), jnp.float32), 0.1, 1.9)
    query_matrix = scatter_about(key_list[2], (D, HEADS * HEAD_DIM), D ** -0.5, 0.09375, ((1, 4),))
    forget_gate_matrix = scatter_about(key_list[3], (D, HEADS * HEAD_DIM), D ** -0.5, 0.09375, ((1, 4),))
    value_matrix = scatter_about(key_list[4], (D, HEADS * HEAD_DIM), D ** -0.5, 0.09375, ((1, 4),))
    forget_floor_channel = jnp.clip(0.02 + 0.93 * jax.random.uniform(key_list[5], (HEADS * HEAD_DIM,), jnp.float32) ** levels(key_list[5], (HEADS * HEAD_DIM,), ((0, 4),), -0.2, 0.2), 0.02, 0.95)
    proposal_extra_decay = draw_proposal_extra_decay(jax.random.fold_in(key_list[10], 71), 0)
    prior_proposal_states = scatter_about(key_list[7], (SEQS, PROPOSALS, HEADS * HEAD_DIM, HEAD_DIM), 0.5, 4.0, ((0, 8), (2, 4)), jnp.float32)
    accepted = plant(jax.random.randint(key_list[8], (SEQS,), 1, PROPOSALS + 1), jax.random.fold_in(key_list[8], 1), 1, PROPOSALS).astype(jnp.int32)
    output_matrix = scatter_about(key_list[9], (HEADS * HEAD_DIM, D), (25 * HEADS * HEAD_DIM) ** -0.5, 0.02734375, ((0, 4), (1, 8)))
    return dict(proposals=proposals, input_norm_gain=input_norm_gain, query_matrix=query_matrix, forget_gate_matrix=forget_gate_matrix, value_matrix=value_matrix, forget_floor_channel=forget_floor_channel, proposal_extra_decay=proposal_extra_decay, prior_proposal_states=prior_proposal_states, accepted=accepted, output_matrix=output_matrix)


def reference(proposals, input_norm_gain, query_matrix, forget_gate_matrix, value_matrix, forget_floor_channel, proposal_extra_decay, prior_proposal_states, accepted, output_matrix):
    seq_count, prop_count, model_width = proposals.shape
    flat_rows = proposals.reshape(seq_count * prop_count, model_width).astype(jnp.float32)
    row_scale = lax.rsqrt(lax.optimization_barrier(jnp.mean(flat_rows * flat_rows, axis=1)) + 1e-06)[:, None]
    scaled = (flat_rows * input_norm_gain).astype(jnp.bfloat16)

    def project(weight):
        return (jnp.dot(scaled, weight, preferred_element_type=jnp.float32) * row_scale).astype(jnp.bfloat16)
    query_pre = project(query_matrix)
    forget_pre = project(forget_gate_matrix)
    value_pre = project(value_matrix)
    head_shape = (seq_count, prop_count, HEADS, HEAD_DIM)
    query_act = jax.nn.silu(query_pre.astype(jnp.float32)).reshape(head_shape)
    lower_part = forget_floor_channel.reshape(HEADS, HEAD_DIM)
    forget_gate = lower_part + (1.0 - lower_part) * jax.nn.sigmoid(forget_pre.astype(jnp.float32).reshape(head_shape))
    forget_gate_logs = jnp.log(forget_gate) + proposal_extra_decay[:, :, :, None]
    key_part = 1.0 - forget_gate
    values = value_pre.astype(jnp.float32).reshape(head_shape)
    picked = jnp.take_along_axis(prior_proposal_states, (accepted - 1).astype(jnp.int32)[:, None, None, None], axis=1)[:, 0]
    carried = picked.reshape(seq_count, HEADS, HEAD_DIM, HEAD_DIM)
    snapshots = []
    outputs = []
    for position in range(PROPOSALS):
        carried = jnp.exp(forget_gate_logs[:, position])[:, :, None, :] * carried + values[:, position][:, :, :, None] * key_part[:, position][:, :, None, :]
        outputs.append(jnp.einsum('shvk,shk->shv', carried, query_act[:, position]))
        snapshots.append(carried.reshape(seq_count, HEADS * HEAD_DIM, HEAD_DIM))
    mixed_rows = jnp.stack(outputs, axis=1).reshape(seq_count * prop_count, HEADS * HEAD_DIM)
    gated_rows = mixed_rows.astype(jnp.bfloat16)
    result = jnp.dot(gated_rows, output_matrix, preferred_element_type=jnp.float32).astype(jnp.bfloat16)
    return (result.reshape(seq_count, prop_count, model_width), jnp.stack(snapshots, axis=1))
```

```python
import functools

import jax
import jax.numpy as jnp
from jax import lax
from jax.experimental import pallas as pl
from jax.experimental.pallas import tpu as pltpu
from jax.sharding import PartitionSpec as P

MESH = pl.DeviceIdType.MESH


def layer_kernel(
    kv_size, tp_size, chunk,
    prop, gain, wq, wf, wv, floor, ped, acc, states, wo,
    out, snap,
    xbuf, gbuf, fbuf, pbuf, wbuf, sbuf, wobuf, scaled, vcol, gath, part, precv,
    lsem, wsem, ssem, xs_sem, xr_sem, gs_sem, gr_sem, ps_sem, pr_sem,
):
    my_kv = lax.axis_index("kv")
    my_tp = lax.axis_index("tp")
    seqs, steps, block = prop.shape
    rows = seqs * steps
    depth, width = wq.shape
    key_dim = states.shape[3]
    heads = width // key_dim
    chunks = depth // chunk
    weights = (wq, wf, wv)

    own_prop = pltpu.make_async_copy(prop, xbuf.at[my_tp], lsem.at[0])
    own_prop.start()
    small = [
        pltpu.make_async_copy(gain, gbuf, lsem.at[1]),
        pltpu.make_async_copy(floor, fbuf, lsem.at[2]),
        pltpu.make_async_copy(ped, pbuf, lsem.at[3]),
    ]
    for copy in small:
        copy.start()

    def weight_copy(which, index):
        at = index * chunk if isinstance(index, int) else pl.multiple_of(index * chunk, chunk)
        return pltpu.make_async_copy(
            weights[which].at[pl.ds(at, chunk)], wbuf.at[which, index], wsem.at[which, index]
        )

    for index in range(chunks):
        for which in range(3):
            weight_copy(which, index).start()
    state_copy = pltpu.make_async_copy(states, sbuf, ssem.at[0])
    state_copy.start()
    wo_copy = pltpu.make_async_copy(wo, wobuf, ssem.at[1])
    wo_copy.start()

    def tp_peer(step):
        return lax.rem(my_tp + step, tp_size)

    def kv_peer(step):
        return lax.rem(my_kv + step, kv_size)

    barrier = pltpu.get_barrier_semaphore()
    for step in range(1, tp_size):
        pl.semaphore_signal(barrier, inc=1, device_id=(my_kv, tp_peer(step)), device_id_type=MESH)
    for step in range(1, kv_size):
        pl.semaphore_signal(barrier, inc=1, device_id=(kv_peer(step), my_tp), device_id_type=MESH)
    pl.semaphore_wait(barrier, tp_size + kv_size - 2)

    own_prop.wait()

    def prop_copy(step):
        return pltpu.make_async_remote_copy(
            src_ref=xbuf.at[my_tp],
            dst_ref=xbuf.at[my_tp],
            send_sem=xs_sem.at[step],
            recv_sem=xr_sem.at[my_tp],
            device_id=(my_kv, tp_peer(step)),
            device_id_type=MESH,
        )

    for step in range(1, tp_size):
        prop_copy(step).start()
    for copy in small:
        copy.wait()
    for step in range(1, tp_size):
        source = tp_peer(step)
        pltpu.make_async_remote_copy(
            src_ref=xbuf.at[source],
            dst_ref=xbuf.at[source],
            send_sem=xs_sem.at[step],
            recv_sem=xr_sem.at[source],
            device_id=(my_kv, source),
            device_id_type=MESH,
        ).wait_recv()

    squares = jnp.zeros((rows, chunk), jnp.float32)
    for index in range(chunks):
        owner, at = divmod(index * chunk, block)
        x = jnp.concatenate(
            [xbuf[owner, s, :, at : at + chunk].astype(jnp.float32) for s in range(seqs)], axis=0
        )
        squares = squares + x * x
        g = gbuf[:, index * chunk : (index + 1) * chunk]
        scaled[index] = (x * g).astype(jnp.bfloat16)
    mean = jnp.sum(squares, axis=1, keepdims=True) * (1.0 / depth)
    row_scale = lax.rsqrt(mean + 1e-06)

    def project(index, totals):
        left = scaled[index]
        added = []
        for which in range(3):
            weight_copy(which, index).wait()
            added.append(
                totals[which]
                + jnp.dot(left, wbuf[which, index], preferred_element_type=jnp.float32)
            )
        return tuple(added)

    zero = jnp.zeros((rows, width), jnp.float32)
    totals = lax.fori_loop(0, chunks, project, (zero, zero, zero))
    query_pre, forget_pre, values = [
        (total * row_scale).astype(jnp.bfloat16).astype(jnp.float32) for total in totals
    ]
    query = query_pre * (1.0 / (1.0 + jnp.exp(-query_pre)))
    low = fbuf[...]
    forget = low + (1.0 - low) * (1.0 / (1.0 + jnp.exp(-forget_pre)))
    key = 1.0 - forget
    extra = jnp.exp(jnp.concatenate([pbuf[s] for s in range(seqs)], axis=0))
    extra = jnp.concatenate(
        [jnp.broadcast_to(extra[:, h : h + 1], (rows, key_dim)) for h in range(heads)], axis=1
    )
    decay = forget * extra

    row = lax.broadcasted_iota(jnp.int32, (rows, 1), 0)
    place = lax.rem(row, steps)
    reach = query
    start_query = query
    mixed = jnp.zeros((rows, width), jnp.float32)
    for lag in range(steps):
        lag_key = pltpu.roll(key, lag, 0) if lag else key
        lag_value = pltpu.roll(values, lag, 0) if lag else values
        lag_decay = pltpu.roll(decay, lag, 0) if lag else decay
        product = reach * lag_key
        score = jnp.concatenate(
            [
                jnp.broadcast_to(
                    jnp.sum(product[:, h * key_dim : (h + 1) * key_dim], axis=1, keepdims=True),
                    (rows, key_dim),
                )
                for h in range(heads)
            ],
            axis=1,
        )
        mixed = mixed + jnp.where(place >= lag, score * lag_value, 0.0)
        reach = reach * lag_decay
        start_query = jnp.where(place == lag, reach, start_query)
    start_query = start_query.astype(jnp.bfloat16)

    state_copy.wait()
    parts = []
    for h in range(heads):
        lanes = slice(h * key_dim, (h + 1) * key_dim)
        total = mixed[:, lanes]
        for s in range(seqs):
            state = sbuf[s, jnp.maximum(acc[s] - 1, 0), lanes, :]
            seen = lax.dot_general(
                start_query[:, lanes],
                state.astype(jnp.bfloat16),
                (((1,), (1,)), ((), ())),
                preferred_element_type=jnp.float32,
            )
            inside = (row >= s * steps) & (row < (s + 1) * steps)
            total = total + jnp.where(inside, seen, 0.0)
        parts.append(total)
    gath[my_kv] = jnp.concatenate(parts, axis=1).astype(jnp.bfloat16)

    def gated_copy(step):
        return pltpu.make_async_remote_copy(
            src_ref=gath.at[my_kv],
            dst_ref=gath.at[my_kv],
            send_sem=gs_sem.at[step],
            recv_sem=gr_sem.at[my_kv],
            device_id=(kv_peer(step), my_tp),
            device_id_type=MESH,
        )

    for step in range(1, kv_size):
        gated_copy(step).start()

    vcol[...] = values.T
    for s in range(seqs):
        for h in range(heads):
            lanes = slice(h * key_dim, (h + 1) * key_dim)
            state = sbuf[s, jnp.maximum(acc[s] - 1, 0), lanes, :]
            for t in range(steps):
                r = s * steps + t
                state = (
                    decay[r : r + 1, lanes] * state
                    + vcol[lanes, r : r + 1] * key[r : r + 1, lanes]
                )
                snap[s, t, lanes, :] = state

    wo_copy.wait()
    per_tp = kv_size // tp_size

    def partial_for(target):
        for i in range(per_tp):
            source = target * per_tp + i

            @pl.when(source != my_kv)
            def _():
                pltpu.make_async_remote_copy(
                    src_ref=gath.at[source],
                    dst_ref=gath.at[source],
                    send_sem=gs_sem.at[0],
                    recv_sem=gr_sem.at[source],
                    device_id=(source, my_tp),
                    device_id_type=MESH,
                ).wait_recv()

        left = jnp.concatenate(
            [gath[target * per_tp + i].astype(jnp.float32) for i in range(per_tp)], axis=0
        ).astype(jnp.bfloat16)
        return jnp.dot(left, wobuf[...], preferred_element_type=jnp.float32)

    def part_copy(step):
        return pltpu.make_async_remote_copy(
            src_ref=part.at[step],
            dst_ref=precv.at[my_tp],
            send_sem=ps_sem.at[step],
            recv_sem=pr_sem.at[my_tp],
            device_id=(my_kv, tp_peer(step)),
            device_id_type=MESH,
        )

    for step in range(1, tp_size):
        part[step] = partial_for(tp_peer(step)).astype(jnp.bfloat16)
        part_copy(step).start()
    total = partial_for(my_tp)
    for step in range(1, tp_size):
        source = tp_peer(step)
        pltpu.make_async_remote_copy(
            src_ref=part.at[step],
            dst_ref=precv.at[source],
            send_sem=ps_sem.at[step],
            recv_sem=pr_sem.at[source],
            device_id=(my_kv, source),
            device_id_type=MESH,
        ).wait_recv()
        total = total + precv[source].astype(jnp.float32)
    for s in range(out.shape[0]):
        out[s] = total[s * steps : (s + 1) * steps].astype(out.dtype)

    for step in range(1, tp_size):
        prop_copy(step).wait_send()
        part_copy(step).wait_send()
    for step in range(1, kv_size):
        gated_copy(step).wait_send()


def per_device(kv_size, tp_size, proposals, gain, wq, wf, wv, floor, ped, states, accepted, wo):
    seqs, steps, block = proposals.shape
    rows = seqs * steps
    depth, width = wq.shape
    key_dim = states.shape[3]
    features = wo.shape[1]
    out_seqs = seqs * kv_size // tp_size
    chunk = 512
    chunks = depth // chunk
    anywhere = pl.BlockSpec(memory_space=pl.ANY)
    vmem = pl.BlockSpec(memory_space=pltpu.VMEM)
    smem = pl.BlockSpec(memory_space=pltpu.SMEM)
    dma = pltpu.SemaphoreType.DMA
    return pl.pallas_call(
        functools.partial(layer_kernel, kv_size, tp_size, chunk),
        out_shape=(
            jax.ShapeDtypeStruct((out_seqs, steps, features), jnp.bfloat16),
            jax.ShapeDtypeStruct(states.shape, jnp.float32),
        ),
        in_specs=[anywhere] * 7 + [smem] + [anywhere] * 2,
        out_specs=(vmem, vmem),
        scratch_shapes=[
            pltpu.VMEM((tp_size, seqs, steps, block), jnp.bfloat16),
            pltpu.VMEM((1, depth), jnp.float32),
            pltpu.VMEM((1, width), jnp.float32),
            pltpu.VMEM(ped.shape, jnp.float32),
            pltpu.VMEM((3, chunks, chunk, width), jnp.bfloat16),
            pltpu.VMEM(states.shape, jnp.float32),
            pltpu.VMEM(wo.shape, jnp.bfloat16),
            pltpu.VMEM((chunks, rows, chunk), jnp.bfloat16),
            pltpu.VMEM((width, rows), jnp.float32),
            pltpu.VMEM((kv_size, rows, width), jnp.bfloat16),
            pltpu.VMEM((tp_size, out_seqs * steps, features), jnp.bfloat16),
            pltpu.VMEM((tp_size, out_seqs * steps, features), jnp.bfloat16),
            dma((4,)),
            dma((3, chunks)),
            dma((2,)),
            dma((tp_size,)),
            dma((tp_size,)),
            dma((kv_size,)),
            dma((kv_size,)),
            dma((tp_size,)),
            dma((tp_size,)),
        ],
        compiler_params=pltpu.CompilerParams(collective_id=0, has_side_effects=True),
    )(
        proposals, gain.reshape(1, depth), wq, wf, wv, floor.reshape(1, width), ped, accepted,
        states, wo,
    )


def solution(mesh):
    placed = (
        P("kv", None, "tp"),
        P(),
        P(None, "tp"),
        P(None, "tp"),
        P(None, "tp"),
        P("tp"),
        P("kv", None, "tp"),
        P("kv", None, "tp", None),
        P("kv"),
        P("tp", "kv"),
    )
    return jax.shard_map(
        functools.partial(per_device, mesh.shape["kv"], mesh.shape["tp"]),
        mesh=mesh,
        in_specs=placed,
        out_specs=(P("tp", None, "kv"), P("kv", None, "tp", None)),
        check_vma=False,
    )
```

```python
import functools

import jax
import jax.numpy as jnp
from jax import lax
from jax.experimental import pallas as pl
from jax.experimental.pallas import tpu as pltpu
from jax.sharding import PartitionSpec as P

MESH = pl.DeviceIdType.MESH


def layer_kernel(
    kv_size, tp_size, chunk,
    prop, gain, wq, wf, wv, floor, ped, accepted, states, wo,
    out, snap,
    acc, xbuf, gbuf, fbuf, pbuf, wbuf, sbuf, wobuf, scaled, vcol, gath, part, precv, own,
    lsem, wsem, ssem, xs_sem, xr_sem, gs_sem, gr_sem, ps_sem, pr_sem,
):
    my_kv = lax.axis_index("kv")
    my_tp = lax.axis_index("tp")
    seqs, steps, block = prop.shape
    rows = seqs * steps
    depth, width = wq.shape
    key_dim = states.shape[3]
    heads = width // key_dim
    chunks = depth // chunk
    weights = (wq, wf, wv)

    def tp_peer(step):
        return lax.rem(my_tp + step, tp_size)

    def kv_peer(step):
        return lax.rem(my_kv + step, kv_size)

    barrier = pltpu.get_barrier_semaphore()
    for step in range(1, tp_size):
        pl.semaphore_signal(barrier, inc=1, device_id=(my_kv, tp_peer(step)), device_id_type=MESH)
    for step in range(1, kv_size):
        pl.semaphore_signal(barrier, inc=1, device_id=(kv_peer(step), my_tp), device_id_type=MESH)
    own_prop = pltpu.make_async_copy(prop, xbuf.at[my_tp], lsem.at[0])
    own_prop.start()
    small = [
        pltpu.make_async_copy(gain, gbuf, lsem.at[1]),
        pltpu.make_async_copy(floor, fbuf, lsem.at[2]),
        pltpu.make_async_copy(ped, pbuf, lsem.at[3]),
        pltpu.make_async_copy(accepted, acc, lsem.at[4]),
    ]
    for copy in small:
        copy.start()

    def weight_copy(which, index):
        at = index * chunk if isinstance(index, int) else pl.multiple_of(index * chunk, chunk)
        return pltpu.make_async_copy(
            weights[which].at[pl.ds(at, chunk)], wbuf.at[which, index], wsem.at[which, index]
        )

    for index in range(chunks):
        for which in range(3):
            weight_copy(which, index).start()
    state_copy = pltpu.make_async_copy(states, sbuf, ssem.at[0])
    state_copy.start()
    wo_copy = pltpu.make_async_copy(wo, wobuf, ssem.at[1])
    wo_copy.start()

    pl.semaphore_wait(barrier, tp_size + kv_size - 2)

    own_prop.wait()

    def prop_copy(step):
        return pltpu.make_async_remote_copy(
            src_ref=xbuf.at[my_tp],
            dst_ref=xbuf.at[my_tp],
            send_sem=xs_sem.at[step],
            recv_sem=xr_sem.at[my_tp],
            device_id=(my_kv, tp_peer(step)),
            device_id_type=MESH,
        )

    for step in range(1, tp_size):
        prop_copy(step).start()
    for copy in small:
        copy.wait()
    for step in range(1, tp_size):
        source = tp_peer(step)
        pltpu.make_async_remote_copy(
            src_ref=xbuf.at[source],
            dst_ref=xbuf.at[source],
            send_sem=xs_sem.at[step],
            recv_sem=xr_sem.at[source],
            device_id=(my_kv, source),
            device_id_type=MESH,
        ).wait_recv()

    squares = jnp.zeros((rows, chunk), jnp.float32)
    for index in range(chunks):
        owner, at = divmod(index * chunk, block)
        x = jnp.concatenate(
            [xbuf[owner, s, :, at : at + chunk].astype(jnp.float32) for s in range(seqs)], axis=0
        )
        squares = squares + x * x
        g = gbuf[:, index * chunk : (index + 1) * chunk]
        scaled[index] = (x * g).astype(jnp.bfloat16)
    mean = jnp.sum(squares, axis=1, keepdims=True) * (1.0 / depth)
    row_scale = lax.rsqrt(mean + 1e-06)

    def project(index, totals):
        left = scaled[index]
        added = []
        for which in range(3):
            weight_copy(which, index).wait()
            added.append(
                totals[which]
                + jnp.dot(left, wbuf[which, index], preferred_element_type=jnp.float32)
            )
        return tuple(added)

    zero = jnp.zeros((rows, width), jnp.float32)
    totals = (zero, zero, zero)
    for index in range(chunks):
        totals = project(index, totals)
    query_pre, forget_pre, values = [
        (total * row_scale).astype(jnp.bfloat16).astype(jnp.float32) for total in totals
    ]
    query = query_pre * (1.0 / (1.0 + jnp.exp(-query_pre)))
    low = fbuf[...]
    forget = low + (1.0 - low) * (1.0 / (1.0 + jnp.exp(-forget_pre)))
    key = 1.0 - forget
    extra = jnp.exp(jnp.concatenate([pbuf[s] for s in range(seqs)], axis=0))
    extra = jnp.concatenate(
        [jnp.broadcast_to(extra[:, h : h + 1], (rows, key_dim)) for h in range(heads)], axis=1
    )
    decay = forget * extra

    row = lax.broadcasted_iota(jnp.int32, (rows, 1), 0)
    place = lax.rem(row, steps)
    reach = query
    start_query = query
    mixed = jnp.zeros((rows, width), jnp.float32)
    for lag in range(steps):
        lag_key = pltpu.roll(key, lag, 0) if lag else key
        lag_value = pltpu.roll(values, lag, 0) if lag else values
        lag_decay = pltpu.roll(decay, lag, 0) if lag else decay
        product = reach * lag_key
        score = jnp.concatenate(
            [
                jnp.broadcast_to(
                    jnp.sum(product[:, h * key_dim : (h + 1) * key_dim], axis=1, keepdims=True),
                    (rows, key_dim),
                )
                for h in range(heads)
            ],
            axis=1,
        )
        mixed = mixed + jnp.where(place >= lag, score * lag_value, 0.0)
        reach = reach * lag_decay
        start_query = jnp.where(place == lag, reach, start_query)
    start_query = start_query.astype(jnp.bfloat16)

    state_copy.wait()
    parts = []
    for h in range(heads):
        lanes = slice(h * key_dim, (h + 1) * key_dim)
        total = mixed[:, lanes]
        for s in range(seqs):
            state = sbuf[s, jnp.maximum(acc[s] - 1, 0), lanes, :]
            seen = lax.dot_general(
                start_query[:, lanes],
                state.astype(jnp.bfloat16),
                (((1,), (1,)), ((), ())),
                preferred_element_type=jnp.float32,
            )
            inside = (row >= s * steps) & (row < (s + 1) * steps)
            total = total + jnp.where(inside, seen, 0.0)
        parts.append(total)
    gath[my_kv] = jnp.concatenate(parts, axis=1).astype(jnp.bfloat16)

    def gated_copy(step):
        return pltpu.make_async_remote_copy(
            src_ref=gath.at[my_kv],
            dst_ref=gath.at[my_kv],
            send_sem=gs_sem.at[step],
            recv_sem=gr_sem.at[my_kv],
            device_id=(kv_peer(step), my_tp),
            device_id_type=MESH,
        )

    for step in range(1, kv_size):
        gated_copy(step).start()

    vcol[...] = values.T
    for s in range(seqs):
        for h in range(heads):
            lanes = slice(h * key_dim, (h + 1) * key_dim)
            state = sbuf[s, jnp.maximum(acc[s] - 1, 0), lanes, :]
            for t in range(steps):
                r = s * steps + t
                state = (
                    decay[r : r + 1, lanes] * state
                    + vcol[lanes, r : r + 1] * key[r : r + 1, lanes]
                )
                snap[s, t, lanes, :] = state

    wo_copy.wait()
    per_tp = kv_size // tp_size

    def partial_for(target):
        for i in range(per_tp):
            source = target * per_tp + i

            @pl.when(source != my_kv)
            def _():
                pltpu.make_async_remote_copy(
                    src_ref=gath.at[source],
                    dst_ref=gath.at[source],
                    send_sem=gs_sem.at[0],
                    recv_sem=gr_sem.at[source],
                    device_id=(source, my_tp),
                    device_id_type=MESH,
                ).wait_recv()

        left = jnp.concatenate(
            [gath[target * per_tp + i].astype(jnp.float32) for i in range(per_tp)], axis=0
        ).astype(jnp.bfloat16)
        return jnp.dot(left, wobuf[...], preferred_element_type=jnp.float32)

    def part_copy(target):
        return pltpu.make_async_remote_copy(
            src_ref=part.at[target],
            dst_ref=precv.at[my_tp],
            send_sem=ps_sem.at[target],
            recv_sem=pr_sem.at[my_tp],
            device_id=(my_kv, target),
            device_id_type=MESH,
        )

    base = my_kv // per_tp
    for step in range(tp_size):
        target = lax.rem(base + step, tp_size)
        block_sum = partial_for(target)
        own[target] = block_sum
        part[target] = block_sum.astype(jnp.bfloat16)

        @pl.when(target != my_tp)
        def _():
            part_copy(target).start()

    total = own[my_tp]
    for step in range(1, tp_size):
        source = tp_peer(step)
        pltpu.make_async_remote_copy(
            src_ref=part.at[source],
            dst_ref=precv.at[source],
            send_sem=ps_sem.at[source],
            recv_sem=pr_sem.at[source],
            device_id=(my_kv, source),
            device_id_type=MESH,
        ).wait_recv()
        total = total + precv[source].astype(jnp.float32)
    for s in range(out.shape[0]):
        out[s] = total[s * steps : (s + 1) * steps].astype(out.dtype)

    for step in range(1, tp_size):
        prop_copy(step).wait_send()
        part_copy(tp_peer(step)).wait_send()
    for step in range(1, kv_size):
        gated_copy(step).wait_send()


def per_device(kv_size, tp_size, proposals, gain, wq, wf, wv, floor, ped, states, accepted, wo):
    seqs, steps, block = proposals.shape
    rows = seqs * steps
    depth, width = wq.shape
    key_dim = states.shape[3]
    features = wo.shape[1]
    out_seqs = seqs * kv_size // tp_size
    chunk = 512
    chunks = depth // chunk
    anywhere = pl.BlockSpec(memory_space=pl.ANY)
    vmem = pl.BlockSpec(memory_space=pltpu.VMEM)
    dma = pltpu.SemaphoreType.DMA
    return pl.pallas_call(
        functools.partial(layer_kernel, kv_size, tp_size, chunk),
        out_shape=(
            pltpu.VMEM((out_seqs, steps, features), jnp.bfloat16),
            pltpu.VMEM(states.shape, jnp.float32),
        ),
        in_specs=[anywhere] * 10,
        out_specs=(vmem, vmem),
        scratch_shapes=[
            pltpu.SMEM(accepted.shape, jnp.int32),
            pltpu.VMEM((tp_size, seqs, steps, block), jnp.bfloat16),
            pltpu.VMEM((1, depth), jnp.float32),
            pltpu.VMEM((1, width), jnp.float32),
            pltpu.VMEM(ped.shape, jnp.float32),
            pltpu.VMEM((3, chunks, chunk, width), jnp.bfloat16),
            pltpu.VMEM(states.shape, jnp.float32),
            pltpu.VMEM(wo.shape, jnp.bfloat16),
            pltpu.VMEM((chunks, rows, chunk), jnp.bfloat16),
            pltpu.VMEM((width, rows), jnp.float32),
            pltpu.VMEM((kv_size, rows, width), jnp.bfloat16),
            pltpu.VMEM((tp_size, out_seqs * steps, features), jnp.bfloat16),
            pltpu.VMEM((tp_size, out_seqs * steps, features), jnp.bfloat16),
            pltpu.VMEM((tp_size, out_seqs * steps, features), jnp.float32),
            dma((5,)),
            dma((3, chunks)),
            dma((2,)),
            dma((tp_size,)),
            dma((tp_size,)),
            dma((kv_size,)),
            dma((kv_size,)),
            dma((tp_size,)),
            dma((tp_size,)),
        ],
        compiler_params=pltpu.CompilerParams(collective_id=0, has_side_effects=True),
    )(
        proposals, gain.reshape(1, depth), wq, wf, wv, floor.reshape(1, width), ped, accepted,
        states, wo,
    )


def solution(mesh):
    placed = (
        P("kv", None, "tp"),
        P(),
        P(None, "tp"),
        P(None, "tp"),
        P(None, "tp"),
        P("tp"),
        P("kv", None, "tp"),
        P("kv", None, "tp", None),
        P("kv"),
        P("tp", "kv"),
    )
    return jax.shard_map(
        functools.partial(per_device, mesh.shape["kv"], mesh.shape["tp"]),
        mesh=mesh,
        in_specs=placed,
        out_specs=(P("tp", None, "kv"), P("kv", None, "tp", None)),
        check_vma=False,
    )
```

```python
import functools

import jax
import jax.numpy as jnp
from jax import lax
from jax.experimental import pallas as pl
from jax.experimental.pallas import tpu as pltpu
from jax.sharding import PartitionSpec as P

MESH = pl.DeviceIdType.MESH


def layer_kernel(
    kv_size, tp_size, chunk,
    prop, gain, wq, wf, wv, floor, ped, accepted, states, wo,
    out, snap,
    acc, xbuf, gbuf, fbuf, pbuf, wbuf, sbuf, wobuf, scaled, vcol, gath, part, precv, own,
    lsem, wsem, ssem, xs_sem, xr_sem, gs_sem, gr_sem, ps_sem, pr_sem,
):
    my_kv = lax.axis_index("kv")
    my_tp = lax.axis_index("tp")
    seqs, steps, block = prop.shape
    rows = seqs * steps
    depth, width = wq.shape
    key_dim = states.shape[3]
    heads = width // key_dim
    chunks = depth // chunk
    weights = (wf, wq, wv)

    def tp_peer(step):
        return lax.rem(my_tp + step, tp_size)

    def kv_peer(step):
        return lax.rem(my_kv + step, kv_size)

    barrier = pltpu.get_barrier_semaphore()
    for step in range(1, tp_size):
        pl.semaphore_signal(barrier, inc=1, device_id=(my_kv, tp_peer(step)), device_id_type=MESH)
    for step in range(1, kv_size):
        pl.semaphore_signal(barrier, inc=1, device_id=(kv_peer(step), my_tp), device_id_type=MESH)
    own_prop = pltpu.make_async_copy(prop, xbuf.at[my_tp], lsem.at[0])
    own_prop.start()
    small = [
        pltpu.make_async_copy(gain, gbuf, lsem.at[1]),
        pltpu.make_async_copy(floor, fbuf, lsem.at[2]),
        pltpu.make_async_copy(ped, pbuf, lsem.at[3]),
        pltpu.make_async_copy(accepted, acc, lsem.at[4]),
    ]
    for copy in small:
        copy.start()

    def weight_copy(which, index):
        at = index * chunk if isinstance(index, int) else pl.multiple_of(index * chunk, chunk)
        return pltpu.make_async_copy(
            weights[which].at[pl.ds(at, chunk)], wbuf.at[which, index], wsem.at[which, index]
        )

    state_copy = pltpu.make_async_copy(states, sbuf, ssem.at[0])
    for which in range(3):
        if which == 2:
            state_copy.start()
        for index in range(chunks):
            weight_copy(which, index).start()
    wo_copy = pltpu.make_async_copy(wo, wobuf, ssem.at[1])
    wo_copy.start()

    pl.semaphore_wait(barrier, tp_size + kv_size - 2)

    own_prop.wait()

    def prop_copy(step):
        return pltpu.make_async_remote_copy(
            src_ref=xbuf.at[my_tp],
            dst_ref=xbuf.at[my_tp],
            send_sem=xs_sem.at[step],
            recv_sem=xr_sem.at[my_tp],
            device_id=(my_kv, tp_peer(step)),
            device_id_type=MESH,
        )

    for step in range(1, tp_size):
        prop_copy(step).start()
    for copy in small:
        copy.wait()
    for step in range(1, tp_size):
        source = tp_peer(step)
        pltpu.make_async_remote_copy(
            src_ref=xbuf.at[source],
            dst_ref=xbuf.at[source],
            send_sem=xs_sem.at[step],
            recv_sem=xr_sem.at[source],
            device_id=(my_kv, source),
            device_id_type=MESH,
        ).wait_recv()

    squares = jnp.zeros((rows, block), jnp.float32)
    for owner in range(tp_size):
        features = slice(owner * block, (owner + 1) * block)
        x = jnp.concatenate(
            [xbuf[owner, s].astype(jnp.float32) for s in range(seqs)], axis=0
        )
        squares = squares + x * x
        scaled[:, features] = (x * gbuf[:, features]).astype(jnp.bfloat16)
    mean = jnp.sum(squares, axis=1, keepdims=True) * (1.0 / depth)
    row_scale = lax.rsqrt(mean + 1e-06)

    def project(which):
        total = jnp.zeros((rows, width), jnp.float32)
        for index in range(chunks):
            weight_copy(which, index).wait()
            total = total + jnp.dot(
                scaled[:, index * chunk : (index + 1) * chunk],
                wbuf[which, index],
                preferred_element_type=jnp.float32,
            )
        return (total * row_scale).astype(jnp.bfloat16).astype(jnp.float32)

    forget_pre = project(0)
    low = fbuf[...]
    forget = low + (1.0 - low) * (1.0 / (1.0 + jnp.exp(-forget_pre)))
    key = 1.0 - forget
    extra = jnp.exp(jnp.concatenate([pbuf[s] for s in range(seqs)], axis=0))
    extra = jnp.concatenate(
        [jnp.broadcast_to(extra[:, h : h + 1], (rows, key_dim)) for h in range(heads)], axis=1
    )
    decay = forget * extra

    query_pre = project(1)
    query = query_pre * (1.0 / (1.0 + jnp.exp(-query_pre)))
    row = lax.broadcasted_iota(jnp.int32, (rows, 1), 0)
    place = lax.rem(row, steps)
    reach = query
    start_query = query
    scores = []
    for lag in range(steps):
        product = reach * (pltpu.roll(key, lag, 0) if lag else key)
        score = jnp.concatenate(
            [
                jnp.broadcast_to(
                    jnp.sum(product[:, h * key_dim : (h + 1) * key_dim], axis=1, keepdims=True),
                    (rows, key_dim),
                )
                for h in range(heads)
            ],
            axis=1,
        )
        scores.append(jnp.where(place >= lag, score, 0.0))
        reach = reach * (pltpu.roll(decay, lag, 0) if lag else decay)
        start_query = jnp.where(place == lag, reach, start_query)
    start_query = start_query.astype(jnp.bfloat16)

    state_copy.wait()
    parts = []
    for h in range(heads):
        lanes = slice(h * key_dim, (h + 1) * key_dim)
        total = jnp.zeros((rows, key_dim), jnp.float32)
        for s in range(seqs):
            state = sbuf[s, jnp.maximum(acc[s] - 1, 0), lanes, :]
            seen = lax.dot_general(
                start_query[:, lanes],
                state.astype(jnp.bfloat16),
                (((1,), (1,)), ((), ())),
                preferred_element_type=jnp.float32,
            )
            inside = (row >= s * steps) & (row < (s + 1) * steps)
            total = total + jnp.where(inside, seen, 0.0)
        parts.append(total)
    mixed = jnp.concatenate(parts, axis=1)

    values = project(2)
    for lag in range(steps):
        mixed = mixed + scores[lag] * (pltpu.roll(values, lag, 0) if lag else values)
    gath[my_kv] = mixed.astype(jnp.bfloat16)

    def gated_copy(step):
        return pltpu.make_async_remote_copy(
            src_ref=gath.at[my_kv],
            dst_ref=gath.at[my_kv],
            send_sem=gs_sem.at[step],
            recv_sem=gr_sem.at[my_kv],
            device_id=(kv_peer(step), my_tp),
            device_id_type=MESH,
        )

    for step in range(1, kv_size):
        gated_copy(step).start()

    vcol[...] = values.T
    for s in range(seqs):
        for h in range(heads):
            lanes = slice(h * key_dim, (h + 1) * key_dim)
            state = sbuf[s, jnp.maximum(acc[s] - 1, 0), lanes, :]
            for t in range(steps):
                r = s * steps + t
                state = (
                    decay[r : r + 1, lanes] * state
                    + vcol[lanes, r : r + 1] * key[r : r + 1, lanes]
                )
                snap[s, t, lanes, :] = state

    wo_copy.wait()
    per_tp = kv_size // tp_size

    def partial_for(target):
        for i in range(per_tp):
            source = target * per_tp + i

            @pl.when(source != my_kv)
            def _():
                pltpu.make_async_remote_copy(
                    src_ref=gath.at[source],
                    dst_ref=gath.at[source],
                    send_sem=gs_sem.at[0],
                    recv_sem=gr_sem.at[source],
                    device_id=(source, my_tp),
                    device_id_type=MESH,
                ).wait_recv()

        left = jnp.concatenate(
            [gath[target * per_tp + i].astype(jnp.float32) for i in range(per_tp)], axis=0
        ).astype(jnp.bfloat16)
        return jnp.dot(left, wobuf[...], preferred_element_type=jnp.float32)

    def part_copy(target):
        return pltpu.make_async_remote_copy(
            src_ref=part.at[target],
            dst_ref=precv.at[my_tp],
            send_sem=ps_sem.at[target],
            recv_sem=pr_sem.at[my_tp],
            device_id=(my_kv, target),
            device_id_type=MESH,
        )

    base = my_kv // per_tp
    for step in range(tp_size):
        target = lax.rem(base + step, tp_size)
        block_sum = partial_for(target)
        own[target] = block_sum
        part[target] = block_sum.astype(jnp.bfloat16)

        @pl.when(target != my_tp)
        def _():
            part_copy(target).start()

    total = own[my_tp]
    for step in range(1, tp_size):
        source = tp_peer(step)
        pltpu.make_async_remote_copy(
            src_ref=part.at[source],
            dst_ref=precv.at[source],
            send_sem=ps_sem.at[source],
            recv_sem=pr_sem.at[source],
            device_id=(my_kv, source),
            device_id_type=MESH,
        ).wait_recv()
        total = total + precv[source].astype(jnp.float32)
    for s in range(out.shape[0]):
        out[s] = total[s * steps : (s + 1) * steps].astype(out.dtype)

    for step in range(1, tp_size):
        prop_copy(step).wait_send()
        part_copy(tp_peer(step)).wait_send()
    for step in range(1, kv_size):
        gated_copy(step).wait_send()


def per_device(kv_size, tp_size, proposals, gain, wq, wf, wv, floor, ped, states, accepted, wo):
    seqs, steps, block = proposals.shape
    rows = seqs * steps
    depth, width = wq.shape
    key_dim = states.shape[3]
    features = wo.shape[1]
    out_seqs = seqs * kv_size // tp_size
    chunk = depth
    chunks = depth // chunk
    anywhere = pl.BlockSpec(memory_space=pl.ANY)
    vmem = pl.BlockSpec(memory_space=pltpu.VMEM)
    dma = pltpu.SemaphoreType.DMA
    return pl.pallas_call(
        functools.partial(layer_kernel, kv_size, tp_size, chunk),
        out_shape=(
            pltpu.VMEM((out_seqs, steps, features), jnp.bfloat16),
            pltpu.VMEM(states.shape, jnp.float32),
        ),
        in_specs=[anywhere] * 10,
        out_specs=(vmem, vmem),
        scratch_shapes=[
            pltpu.SMEM(accepted.shape, jnp.int32),
            pltpu.VMEM((tp_size, seqs, steps, block), jnp.bfloat16),
            pltpu.VMEM((1, depth), jnp.float32),
            pltpu.VMEM((1, width), jnp.float32),
            pltpu.VMEM(ped.shape, jnp.float32),
            pltpu.VMEM((3, chunks, chunk, width), jnp.bfloat16),
            pltpu.VMEM(states.shape, jnp.float32),
            pltpu.VMEM(wo.shape, jnp.bfloat16),
            pltpu.VMEM((rows, depth), jnp.bfloat16),
            pltpu.VMEM((width, rows), jnp.float32),
            pltpu.VMEM((kv_size, rows, width), jnp.bfloat16),
            pltpu.VMEM((tp_size, out_seqs * steps, features), jnp.bfloat16),
            pltpu.VMEM((tp_size, out_seqs * steps, features), jnp.bfloat16),
            pltpu.VMEM((tp_size, out_seqs * steps, features), jnp.float32),
            dma((5,)),
            dma((3, chunks)),
            dma((2,)),
            dma((tp_size,)),
            dma((tp_size,)),
            dma((kv_size,)),
            dma((kv_size,)),
            dma((tp_size,)),
            dma((tp_size,)),
        ],
        compiler_params=pltpu.CompilerParams(collective_id=0, has_side_effects=True),
    )(
        proposals, gain.reshape(1, depth), wq, wf, wv, floor.reshape(1, width), ped, accepted,
        states, wo,
    )


def solution(mesh):
    placed = (
        P("kv", None, "tp"),
        P(),
        P(None, "tp"),
        P(None, "tp"),
        P(None, "tp"),
        P("tp"),
        P("kv", None, "tp"),
        P("kv", None, "tp", None),
        P("kv"),
        P("tp", "kv"),
    )
    return jax.shard_map(
        functools.partial(per_device, mesh.shape["kv"], mesh.shape["tp"]),
        mesh=mesh,
        in_specs=placed,
        out_specs=(P("tp", None, "kv"), P("kv", None, "tp", None)),
        check_vma=False,
    )
```
